32 devices in a mesh: ra: 8 (over z, y), cb: 4 (over x, core).
Axes of the slice: x: 2, y: 2, z: 4, core: 2. Of those that a mesh axis runs over, the one named last changes fastest.
Arguments:
- activations: bfloat16 [512, 4224], P('cb', 'ra'), may hold values from -160 to 160, as said below
- norm_gain: float32 [2, 4224], replicated, may hold values from 0.1 to 1.9
- gate_weight: float32 [2, 4224, 11520], P(None, None, 'ra'), may hold values from -0.09375 to 0.09375
- gate_scale: float32 [2, 11520], P(None, 'ra'), may hold values from 0.3 to 3
- value_weight: float32 [2, 4224, 11520], P(None, None, 'ra'), may hold values from -0.09375 to 0.09375
- value_scale: float32 [2, 11520], P(None, 'ra'), may hold values from 0.3 to 3
- gate_taps: float32 [2, 3, 11520], P(None, None, 'ra'), may hold values from -3 to 3
- value_taps: float32 [2, 3, 11520], P(None, None, 'ra'), may hold values from -3 to 3
- down_weight: float32 [2, 11520, 4224], P(None, None, 'ra'), may hold values from -0.0546875 to 0.0546875
- down_scale: float32 [2, 4224], P(None, 'ra'), may hold values from 0.3 to 3
- final_gain: float32 [4224], P('ra'), may hold values from 0.1 to 1.9
Outputs:
- normalized: bfloat16 [512, 4224], P('cb', 'ra')
The draws below stay inside these ranges and needn't reach their ends.
Inputs may be any that keep to these rules, and one draw needn't show every extreme that they name: `activations`: rows and columns have unequal scales.
All inputs are finite; a program needn't handle non-finite values.
Results may differ from the reference program's by a relative error of at most 0.017.
Values may be sent and summed in bfloat16 or wider, within the bound.
A program may use at most 320 MiB of HBM per device.

```python
import math
import jax
import jax.numpy as jnp
from jax import lax

D = 4224
FF = 11520
LAYERS = 2
CONV = 3
TOKENS = 512


def draw_activations(key, part):
    keys = jax.random.split(key, 2)
    row_scales = jnp.exp(jax.random.uniform(keys[1], (TOKENS, 1), jnp.float32, 0.0, math.log(10.0)))
    column_scales = jnp.exp(jnp.linspace(0.0, math.log(4.0), D, dtype=jnp.float32))
    base = jnp.clip(jax.random.normal(keys[0], (TOKENS, D), jnp.float32), -4.0, 4.0)
    return (base * row_scales * column_scales).astype(jnp.bfloat16)


def block_scale(own_key, extent, pieces, low, top_value):
    gain = 1.0
    for position, blocks in pieces:
        heights = jax.random.uniform(jax.random.fold_in(jax.random.fold_in(own_key, 6), position), (blocks,), jnp.float32, low / len(pieces), top_value / len(pieces))
        gain = gain * jnp.repeat(jnp.exp(heights), extent[position] // blocks).reshape((-1,) + (1,) * (len(extent) - 1 - position))
    return gain


def gaussian(own_key, shape, deviation, limit, pieces=(), kind=jnp.bfloat16):
    array = deviation * jax.random.normal(own_key, shape, jnp.float32)
    if pieces:
        array = array * block_scale(own_key, shape, pieces, -0.22, 0.18)
    return jnp.clip(array, -limit, limit).astype(kind)


def setup_inputs(seed: int = 0) -> dict:
    seeds = jax.random.split(jax.random.key(seed), 12)
    activations = draw_activations(jax.random.fold_in(seeds[11], 71), 0)
    norm_gain = jnp.clip(1.0 + 0.18 * jax.random.normal(seeds[1], (LAYERS, D), jnp.float32), 0.1, 1.9)
    gate_weight = gaussian(seeds[2], (LAYERS, D, FF), D ** -0.5, 0.09375, ((2, 8),), jnp.float32)
    gate_scale = jnp.clip(jnp.exp(math.log(3.0) - 2.3025851 * jax.random.uniform(seeds[3], (LAYERS, FF), jnp.float32) ** block_scale(seeds[3], (LAYERS, FF), ((1, 8),), -0.2, 0.2)), 0.3, 3.0)
    value_weight = gaussian(seeds[4], (LAYERS, D, FF), D ** -0.5, 0.09375, ((2, 8),), jnp.float32)
    value_scale = jnp.clip(jnp.exp(math.log(3.0) - 2.3025851 * jax.random.uniform(seeds[5], (LAYERS, FF), jnp.float32) ** block_scale(seeds[5], (LAYERS, FF), ((1, 8),), -0.2, 0.2)), 0.3, 3.0)
    gate_taps = gaussian(seeds[6], (LAYERS, CONV, FF), 0.577, 3.0, ((2, 8),), jnp.float32)
    value_taps = gaussian(seeds[7], (LAYERS, CONV, FF), 0.577, 3.0, ((2, 8),), jnp.float32)
    down_weight = gaussian(seeds[8], (LAYERS, FF, D), FF ** -0.5, 0.0546875, ((2, 8),), jnp.float32)
    down_scale = jnp.clip(jnp.exp(math.log(3.0) - 2.3025851 * jax.random.uniform(seeds[9], (LAYERS, D), jnp.float32) ** block_scale(seeds[9], (LAYERS, D), ((1, 8),), -0.2, 0.2)), 0.3, 3.0)
    final_gain = jnp.clip(1.0 + 0.18 * jax.random.normal(seeds[10], (D,), jnp.float32), 0.1, 1.9)
    return dict(activations=activations, norm_gain=norm_gain, gate_weight=gate_weight, gate_scale=gate_scale, value_weight=value_weight, value_scale=value_scale, gate_taps=gate_taps, value_taps=value_taps, down_weight=down_weight, down_scale=down_scale, final_gain=final_gain)


epsilon = 1e-06
resid_scale = 0.5

def conv_causal(values_in, tap_weights):
    seq_len = values_in.shape[0]
    taps = tap_weights.shape[0]
    padded = jnp.pad(values_in, ((taps - 1, 0), (0, 0)))
    total = jnp.zeros(values_in.shape, jnp.float32)
    for offset in range(taps):
        total = total + tap_weights[offset] * padded[offset:offset + seq_len]
    return total

def reference(activations, norm_gain, gate_weight, gate_scale, value_weight, value_scale, gate_taps, value_taps, down_weight, down_scale, final_gain):
    tok_rows = activations
    for layer_idx in range(LAYERS):
        wide_rows = tok_rows.astype(jnp.float32)
        inv_norm = lax.rsqrt(lax.optimization_barrier(jnp.mean(wide_rows * wide_rows, axis=1, keepdims=True)) + epsilon)
        scaled = (wide_rows * norm_gain[layer_idx]).astype(jnp.bfloat16)
        gate_pre = jnp.dot(scaled, gate_weight[layer_idx].astype(jnp.bfloat16), preferred_element_type=jnp.float32) * inv_norm * gate_scale[layer_idx]
        value_pre = jnp.dot(scaled, value_weight[layer_idx].astype(jnp.bfloat16), preferred_element_type=jnp.float32) * inv_norm * value_scale[layer_idx]
        gate_conv = conv_causal(gate_pre, gate_taps[layer_idx])
        value_conv = conv_causal(value_pre, value_taps[layer_idx])
        hidden = (jax.nn.silu(gate_conv) * value_conv).astype(jnp.bfloat16)
        down = jnp.dot(hidden, down_weight[layer_idx].astype(jnp.bfloat16), preferred_element_type=jnp.float32)
        tok_rows = (resid_scale * wide_rows + down * down_scale[layer_idx]).astype(jnp.bfloat16)
    wide_rows = tok_rows.astype(jnp.float32)
    inv_norm = lax.rsqrt(lax.optimization_barrier(jnp.mean(wide_rows * wide_rows, axis=1, keepdims=True)) + epsilon)
    return (wide_rows * inv_norm * final_gain).astype(jnp.bfloat16)
```

```python
import functools

import jax
import jax.numpy as jnp
from jax import lax
from jax.experimental import pallas as pl
from jax.experimental.pallas import tpu as pltpu
from jax.sharding import PartitionSpec as P

D = 4224


epsilon = 1e-06
resid_scale = 0.5


def from_behind(value, axis, by):
    length = lax.axis_size(axis)
    pairs = [(i, i + by) for i in range(length) if 0 <= i + by < length]
    return lax.ppermute(value, axis, pairs)


def conv_local(values_in, earlier, tap_weights):
    seq_len = values_in.shape[0]
    taps = tap_weights.shape[0]
    padded = jnp.concatenate([earlier, values_in], axis=0)
    total = jnp.zeros(values_in.shape, jnp.float32)
    for offset in range(taps):
        total = total + tap_weights[offset] * padded[offset : offset + seq_len]
    return total


def plain_device(
    activations,
    norm_gain,
    gate_weight,
    gate_scale,
    value_weight,
    value_scale,
    gate_taps,
    value_taps,
    down_weight,
    down_scale,
    final_gain,
):
    row_count, width_part = activations.shape
    tok_rows = activations
    layer_count = gate_weight.shape[0]
    taps = gate_taps.shape[1]
    for layer_idx in range(layer_count):
        wide_rows = tok_rows.astype(jnp.float32)
        full_rows = lax.all_gather(tok_rows, "ra", axis=1, tiled=True).astype(jnp.float32)
        inv_norm = lax.rsqrt(jnp.mean(full_rows * full_rows, axis=1, keepdims=True) + epsilon)
        scaled = (full_rows * norm_gain[layer_idx]).astype(jnp.bfloat16)
        gate_pre = (
            jnp.dot(
                scaled,
                gate_weight[layer_idx].astype(jnp.bfloat16),
                preferred_element_type=jnp.float32,
            )
            * inv_norm
            * gate_scale[layer_idx]
        )
        value_pre = (
            jnp.dot(
                scaled,
                value_weight[layer_idx].astype(jnp.bfloat16),
                preferred_element_type=jnp.float32,
            )
            * inv_norm
            * value_scale[layer_idx]
        )
        gate_prev, value_prev = from_behind(
            (gate_pre[row_count - taps + 1 :], value_pre[row_count - taps + 1 :]), "cb", 1
        )
        gate_conv = conv_local(gate_pre, gate_prev, gate_taps[layer_idx])
        value_conv = conv_local(value_pre, value_prev, value_taps[layer_idx])
        down_bf = down_weight[layer_idx].astype(jnp.bfloat16)
        hidden = (jax.nn.silu(gate_conv) * value_conv).astype(jnp.bfloat16)
        down = jnp.dot(
            lax.all_gather(hidden, "ra", axis=1, tiled=True),
            down_bf,
            preferred_element_type=jnp.float32,
        )
        tok_rows = (resid_scale * wide_rows + down * down_scale[layer_idx]).astype(jnp.bfloat16)
    wide_rows = tok_rows.astype(jnp.float32)
    sq_final = lax.psum(jnp.sum(wide_rows * wide_rows, axis=1), "ra")
    inv_norm = lax.rsqrt(sq_final[:, None] / D + epsilon)
    return (wide_rows * inv_norm * final_gain).astype(jnp.bfloat16)


MESH = pl.DeviceIdType.MESH
PIECES = 3
TILES = 6
GV_SLOTS = 3
DOWN_BLOCKS = 10
DOWN_SLOTS = 6


def fused_kernel(
    n,
    cols,
    x_ref,
    gain_ref,
    par_ref,
    dscale_ref,
    fgain_ref,
    wg_hbm,
    wv_hbm,
    wd_hbm,
    out_ref,
    xr,
    halo,
    xs,
    hid,
    gbuf,
    vbuf,
    dbuf,
    acc,
    ssq,
    red,
    gsem,
    vsem,
    dsem,
    xsend,
    xrecv,
    bsend,
    brecv,
    hsend,
    hrecv,
    rsend,
    rrecv,
):
    layers, units, depth = wg_hbm.shape
    width, toks = x_ref.shape
    half = n // 2
    piece = width // PIECES
    tile = units // TILES
    kblock = wd_hbm.shape[2] // DOWN_BLOCKS
    me = lax.axis_index("ra")
    col = lax.axis_index("cb")
    pos = (1 - me % 2) * (me // 2) + (me % 2) * (n - 1 - me // 2)

    def member(p):
        p = (p + n) % n
        b = p // half
        return (1 - b) * (2 * p) + b * (2 * (n - 1 - p) + 1)

    ahead = (member(pos + 1), member(pos - 1))

    def origin(d, h):
        return member(pos - h) if d == 0 else member(pos + h)

    def gv_copies(g):
        l, t, slot = g // TILES, g % TILES, g % GV_SLOTS
        rows = pl.ds(pl.multiple_of(t * tile, 8), tile)
        return (
            pltpu.make_async_copy(wg_hbm.at[l, rows], gbuf.at[slot], gsem.at[slot]),
            pltpu.make_async_copy(wv_hbm.at[l, rows], vbuf.at[slot], vsem.at[slot]),
        )

    def down_copy(g):
        l, k, slot = g // DOWN_BLOCKS, g % DOWN_BLOCKS, g % DOWN_SLOTS
        lanes = pl.ds(pl.multiple_of(k * kblock, 128), kblock)
        return pltpu.make_async_copy(wd_hbm.at[l, :, lanes], dbuf.at[slot], dsem.at[slot])

    def x_rows(owner, s):
        return pl.ds(pl.multiple_of(owner * width + s * piece, 16), piece)

    def x_copy(l, d, h, s, sending):
        rows = x_rows(origin(d, h - sending), s)
        return pltpu.make_async_remote_copy(
            src_ref=xr.at[l, rows],
            dst_ref=xr.at[l, rows],
            send_sem=xsend.at[l, d, h - 1, s],
            recv_sem=xrecv.at[l, d, h - 1, s],
            device_id={"ra": ahead[d]},
            device_id_type=MESH,
        )

    def b_copy(l, d, h, s):
        rows = x_rows(origin(d, h), s)
        return pltpu.make_async_remote_copy(
            src_ref=xr.at[l, rows],
            dst_ref=halo.at[l, rows],
            send_sem=bsend.at[l, d, h, s],
            recv_sem=brecv.at[l, d, h, s],
            device_id={"cb": (col + 1) % cols},
            device_id_type=MESH,
        )

    def h_copy(l, d, h, t, sending):
        rows = pl.ds(pl.multiple_of(origin(d, h - sending) * units + t * tile, 16), tile)
        return pltpu.make_async_remote_copy(
            src_ref=hid.at[l, rows],
            dst_ref=hid.at[l, rows],
            send_sem=hsend.at[l, d, h - 1, t],
            recv_sem=hrecv.at[l, d, h - 1, t],
            device_id={"ra": ahead[d]},
            device_id_type=MESH,
        )

    def red_copy(j, owner):
        return pltpu.make_async_remote_copy(
            src_ref=red.at[owner],
            dst_ref=red.at[owner],
            send_sem=rsend.at[j],
            recv_sem=rrecv.at[j],
            device_id={"ra": (me + j) % n},
            device_id_type=MESH,
        )

    for g in range(GV_SLOTS):
        for c in gv_copies(g):
            c.start()
    for g in range(DOWN_SLOTS):
        down_copy(g).start()

    barrier = pltpu.get_barrier_semaphore()
    for j in range(1, n):
        pl.semaphore_signal(
            barrier, inc=1, device_id={"ra": (me + j) % n}, device_id_type=MESH
        )

    for by in (1, cols - 1):
        pl.semaphore_signal(
            barrier, inc=1, device_id={"cb": (col + by) % cols}, device_id_type=MESH
        )

    mine = pl.ds(pl.multiple_of(me * width, 16), width)
    xr[0, mine, :] = x_ref[...]

    @pl.when(col == 0)
    def _():
        halo[...] = jnp.zeros_like(halo)

    pl.semaphore_wait(barrier, n + 1)

    arrivals = []
    for h in range(1, half + 1):
        for s in range(PIECES):
            for d in range(2):
                if h < half or s % 2 == d:
                    arrivals.append((d, h, s))
    everything = [(0, 0, s) for s in range(PIECES)] + arrivals

    def absorb(l, d, h, s, part):
        rows = x_rows(origin(d, h), s)
        wide = (halo if part else xr)[l, rows, :].astype(jnp.float32)
        lanes = slice(part * toks, (part + 1) * toks)
        xs[rows, lanes] = (wide * gain_ref[l, rows, :]).astype(jnp.bfloat16)
        ssq[:, lanes] = ssq[:, lanes] + jnp.sum(wide * wide, axis=0, keepdims=True)

    def absorb_halo(l, d, h, s):
        @pl.when(col > 0)
        def _():
            b_copy(l, d, h, s).wait_recv()

        absorb(l, d, h, s, 1)

    def send_halo(l, d, h, s):
        @pl.when(col < cols - 1)
        def _():
            b_copy(l, d, h, s).start()

    def layer(l, carry):
        for s in range(PIECES):
            for d in range(2):
                x_copy(l, d, 1, s, 1).start()
        for s in range(PIECES):
            send_halo(l, 0, 0, s)
        ssq[...] = jnp.zeros_like(ssq)
        for s in range(PIECES):
            absorb(l, 0, 0, s, 0)
        lag = 4
        for i, (d, h, s) in enumerate(arrivals):
            x_copy(l, d, h, s, 0).wait_recv()
            if h + 1 < half or (h + 1 == half and s % 2 == d):
                x_copy(l, d, h + 1, s, 1).start()
            send_halo(l, d, h, s)
            absorb(l, d, h, s, 0)
            if i >= lag:
                absorb_halo(l, *everything[i - lag])
        for i in range(len(arrivals) - lag, len(everything)):
            absorb_halo(l, *everything[i])

        inv = lax.rsqrt(ssq[...] / depth + epsilon)

        def tail(value, tap, rows):
            prev, own = value[:, :toks], value[:, toks:]
            lane = lax.broadcasted_iota(jnp.int32, own.shape, 1)
            total = par_ref[l, rows, tap + 2 : tap + 3] * own
            for by in (1, 2):
                moved = jnp.where(
                    lane < by, pltpu.roll(prev, by, 1), pltpu.roll(own, by, 1)
                )
                total = total + par_ref[l, rows, tap + 2 - by : tap + 3 - by] * moved
            return total

        def step(i, carry):
            @pl.when(i < TILES)
            def _():
                g = l * TILES + i
                slot = g % GV_SLOTS
                rows = pl.ds(pl.multiple_of(i * tile, 8), tile)
                for c in gv_copies(g):
                    c.wait()
                gate = jnp.dot(
                    gbuf[slot].astype(jnp.bfloat16), xs[...], preferred_element_type=jnp.float32
                )
                gate = gate * inv * par_ref[l, rows, 0:1]
                gate_conv = tail(jnp.concatenate([gate[:, toks:], gate[:, :toks]], 1), 2, rows)
                value = jnp.dot(
                    vbuf[slot].astype(jnp.bfloat16), xs[...], preferred_element_type=jnp.float32
                )
                value = value * inv * par_ref[l, rows, 1:2]
                value_conv = tail(jnp.concatenate([value[:, toks:], value[:, :toks]], 1), 5, rows)
                hidden = gate_conv / (1.0 + jnp.exp(-gate_conv)) * value_conv
                place = pl.ds(pl.multiple_of(me * units + i * tile, 16), tile)
                hid[l, place, :] = hidden.astype(jnp.bfloat16)
                for d in range(2):
                    h_copy(l, d, 1, i, 1).start()

                @pl.when(g + GV_SLOTS < layers * TILES)
                def _():
                    for c in gv_copies(g + GV_SLOTS):
                        c.start()

            for h in range(1, half + 1):
                t = i - h
                inside = (t >= 0) & (t < TILES)
                for d in range(2):
                    even = inside & (t % 2 == d)

                    @pl.when(inside if h < half else even)
                    def _():
                        h_copy(l, d, h, t, 0).wait_recv()

                    if h < half:

                        @pl.when(inside if h + 1 < half else even)
                        def _():
                            h_copy(l, d, h + 1, t, 1).start()

            return carry

        lax.fori_loop(0, TILES + half, step, 0)

        acc[...] = jnp.zeros_like(acc)

        def down_step(k, carry):
            g = l * DOWN_BLOCKS + k
            slot = g % DOWN_SLOTS
            down_copy(g).wait()
            rows = pl.ds(pl.multiple_of(k * kblock, 128), kblock)
            acc[...] += jnp.dot(
                dbuf[slot].astype(jnp.bfloat16),
                hid[l, rows, :],
                preferred_element_type=jnp.float32,
            )

            @pl.when(g + DOWN_SLOTS < layers * DOWN_BLOCKS)
            def _():
                down_copy(g + DOWN_SLOTS).start()

            return carry

        lax.fori_loop(0, DOWN_BLOCKS, down_step, 0)
        wide = xr[l, mine, :].astype(jnp.float32)
        xr[l + 1, mine, :] = (resid_scale * wide + acc[...] * dscale_ref[l]).astype(jnp.bfloat16)
        return carry

    lax.fori_loop(0, layers, layer, 0)

    wide = xr[layers, mine, :].astype(jnp.float32)
    red[me] = jnp.broadcast_to(jnp.sum(wide * wide, axis=0, keepdims=True), red.shape[1:])
    for j in range(1, n):
        red_copy(j, me).start()

    def drain(l, carry):
        for s in range(PIECES):
            for d in range(2):
                for h in range(1, half + 1):
                    if h < half or s % 2 == d:
                        x_copy(l, d, h, s, 1).wait_send()

        @pl.when(col < cols - 1)
        def _():
            for d, h, s in everything:
                b_copy(l, d, h, s).wait_send()

        def drain_tile(t, carry):
            for d in range(2):
                for h in range(1, half):
                    h_copy(l, d, h, t, 1).wait_send()

                @pl.when(t % 2 == d)
                def _():
                    h_copy(l, d, half, t, 1).wait_send()

            return carry

        lax.fori_loop(0, TILES, drain_tile, 0)
        return carry

    lax.fori_loop(0, layers, drain, 0)

    for j in range(1, n):
        red_copy(j, (me + n - j) % n).wait_recv()
    total = jnp.sum(red[:, 0:1, :], axis=0)
    inv = lax.rsqrt(total / depth + epsilon)
    out_ref[...] = (wide * inv * fgain_ref[...]).astype(jnp.bfloat16)
    for j in range(1, n):
        red_copy(j, me).wait_send()


def per_device(
    n,
    cols,
    activations,
    norm_gain,
    gate_weight,
    gate_scale,
    value_weight,
    value_scale,
    gate_taps,
    value_taps,
    down_weight,
    down_scale,
    final_gain,
):
    toks, width = activations.shape
    layers, depth, units = gate_weight.shape
    taps = gate_taps.shape[1]
    hidden = down_weight.shape[1]
    fits = (
        n % 2 == 0
        and n >= 4
        and cols >= 3
        and toks == 128
        and taps == 3
        and width % (16 * PIECES) == 0
        and units % (16 * TILES) == 0
        and depth % 128 == 0
        and hidden % (128 * DOWN_BLOCKS) == 0
    )
    if not fits:
        return plain_device(
            activations,
            norm_gain,
            gate_weight,
            gate_scale,
            value_weight,
            value_scale,
            gate_taps,
            value_taps,
            down_weight,
            down_scale,
            final_gain,
        )
    par = jnp.concatenate(
        [gate_scale[:, None], value_scale[:, None], gate_taps, value_taps], axis=1
    )
    par = jnp.swapaxes(par, 1, 2)
    half = n // 2
    tile = units // TILES
    kblock = hidden // DOWN_BLOCKS
    vm = pl.BlockSpec(memory_space=pltpu.VMEM)
    hbm = pl.BlockSpec(memory_space=pl.ANY)
    dma = pltpu.SemaphoreType.DMA
    out = pl.pallas_call(
        functools.partial(fused_kernel, n, cols),
        out_shape=jax.ShapeDtypeStruct((width, toks), jnp.bfloat16),
        in_specs=[vm] * 5 + [hbm] * 3,
        out_specs=vm,
        scratch_shapes=[
            pltpu.VMEM((layers + 1, depth, toks), jnp.bfloat16),
            pltpu.VMEM((layers, depth, toks), jnp.bfloat16),
            pltpu.VMEM((depth, 2 * toks), jnp.bfloat16),
            pltpu.VMEM((layers, hidden, toks), jnp.bfloat16),
            pltpu.VMEM((GV_SLOTS, tile, depth), jnp.float32),
            pltpu.VMEM((GV_SLOTS, tile, depth), jnp.float32),
            pltpu.VMEM((DOWN_SLOTS, width, kblock), jnp.float32),
            pltpu.VMEM((width, toks), jnp.float32),
            pltpu.VMEM((1, 2 * toks), jnp.float32),
            pltpu.VMEM((n, 8, toks), jnp.float32),
            dma((GV_SLOTS,)),
            dma((GV_SLOTS,)),
            dma((DOWN_SLOTS,)),
            dma((layers, 2, half, PIECES)),
            dma((layers, 2, half, PIECES)),
            dma((layers, 2, half + 1, PIECES)),
            dma((layers, 2, half + 1, PIECES)),
            dma((layers, 2, half, TILES)),
            dma((layers, 2, half, TILES)),
            dma((n,)),
            dma((n,)),
        ],
        compiler_params=pltpu.CompilerParams(
            collective_id=0, has_side_effects=True, vmem_limit_bytes=66 * 1000 * 1000
        ),
    )(
        activations.T,
        norm_gain[:, :, None],
        par,
        down_scale[:, :, None],
        final_gain[:, None],
        jnp.swapaxes(gate_weight, 1, 2),
        jnp.swapaxes(value_weight, 1, 2),
        jnp.swapaxes(down_weight, 1, 2),
    )
    return out.T


def solution(mesh):
    in_specs = (
        P("cb", "ra"),
        P(),
        P(None, None, "ra"),
        P(None, "ra"),
        P(None, None, "ra"),
        P(None, "ra"),
        P(None, None, "ra"),
        P(None, None, "ra"),
        P(None, None, "ra"),
        P(None, "ra"),
        P("ra"),
    )
    out_specs = P("cb", "ra")
    body = functools.partial(per_device, mesh.shape["ra"], mesh.shape["cb"])
    return jax.shard_map(
        body, mesh=mesh, in_specs=in_specs, out_specs=out_specs, check_vma=False
    )
```
